32 devices in a mesh: sp: 8 (over z, x), tp: 4 (over y, core).
Axes of the slice: x: 2, y: 2, z: 4, core: 2. Of those that a mesh axis runs over, the one named last changes fastest.
Arguments:
- queries: bfloat16 [1024, 1024], P('sp', 'tp'), may hold values from -160 to 160
- keys: bfloat16 [1024, 256], P('sp', 'tp'), may hold values from -5 to 5
- values: bfloat16 [1024, 256], P('sp', 'tp'), may hold values from -6 to 6
- cum_gate: float32 [1024, 16], P('sp', 'tp'), as said below
- doc_ids: int32 [1024], P('sp'), may hold values from 0 to 7, never falling along the last dimension, each value on 1 to 640 neighbouring positions
- residual: bfloat16 [1024, 2048], P(('sp', 'tp')), may hold values from -6 to 6
- out_proj: bfloat16 [1024, 2048], replicated, may hold values from -0.1875 to 0.1875
- norm_gain: float32 [2048], replicated, may hold values from 0.1 to 1.9
- route_ids: int32 [1024, 2], P(('sp', 'tp')), may hold values from 0 to 7, all different within a row; in each aligned block of 32 rows (0 to 31, 32 to 63, ...) at most 16 rows name the same one
- route_weights: float32 [1024, 2], P(('sp', 'tp')), may hold values from 0.2 to 1
- expert_gate: bfloat16 [8, 2048, 1024], P('sp', None, 'tp'), may hold values from -0.125 to 0.125
- expert_up: bfloat16 [8, 2048, 1024], P('sp', None, 'tp'), may hold values from -0.125 to 0.125
- expert_down: bfloat16 [8, 1024, 2048], P('sp', 'tp'), may hold values from -0.1875 to 0.1875
Outputs:
- mixed: bfloat16 [1024, 2048], P(('sp', 'tp'))
The draws below stay inside these ranges and needn't reach their ends.
Inputs may be any that keep to these rules, and one draw needn't show every extreme that they name: `route_ids`: within each aligned block of 32 rows no expert is named by more than 16 rows, and in every draw some block has an expert named by exactly 16 rows; the 2 experts of a row differ. `doc_ids`: never falling along positions; a document spans at most 640 positions, and one spans exactly that many. `cum_gate`: never rising along positions.
All inputs are finite; a program needn't handle non-finite values.
Results may differ from the reference program's by a relative error of at most 0.014.
Values may be sent and summed in bfloat16 or wider, within the bound.
A program may use at most 128 MiB of HBM per device.

```python
import math
import jax
import jax.numpy as jnp
import numpy as np
from jax import lax

D = 2048
ASKING_PLANES = 16
HEAD_DIM = 64
KV_HEADS = 4
EXPERT_FF = 1024
TOP = 2
DOCS = 8
TOK_DEV = 128
TEXT_SLOTS = 1024
ROWS_DEV = 32
EXPERTS = 8
CAP = 16
DOC_MOST = 640
N_TP = 4


def shared_keys(key):
    shared = jax.random.fold_in(key, 7)
    drawn = jax.random.normal(jax.random.fold_in(shared, 1), (TEXT_SLOTS, KV_HEADS * HEAD_DIM), jnp.float32)
    drawn = jnp.clip(drawn, -5.0, 5.0)
    return drawn


def draw_keys(key, part):
    drawn = shared_keys(key)
    return drawn.astype(jnp.bfloat16)


def draw_queries(key, part):
    entries = jax.random.normal(jax.random.fold_in(key, 31), (TEXT_SLOTS, ASKING_PLANES * HEAD_DIM), jnp.float32)
    entries = 3.0 * jnp.clip(entries, -6.0, 6.0)
    return entries.astype(jnp.bfloat16)


def draw_cum_gate(key, part):
    lane_number = jax.random.split(jax.random.fold_in(key, 11), 7)
    order = jax.random.permutation(lane_number[0], ASKING_PLANES)
    keeping = ASKING_PLANES // 2
    slow = order < keeping
    slow_total = jax.random.uniform(lane_number[1], (ASKING_PLANES,), jnp.float32, 0.2, 0.8)
    fast_rate = jnp.exp(jax.random.uniform(lane_number[2], (ASKING_PLANES,), jnp.float32, math.log(1.0 / 100.0), math.log(1.0 / 30.0)))
    rate = jnp.where(slow, slow_total / TEXT_SLOTS, fast_rate)
    block_scaling = jnp.exp(jax.random.uniform(lane_number[3], (TEXT_SLOTS // TOK_DEV,), jnp.float32, math.log(0.5), math.log(2.0)))
    block_of = jnp.arange(TEXT_SLOTS, dtype=jnp.int32) // TOK_DEV
    jitter = jax.random.uniform(lane_number[4], (TEXT_SLOTS, ASKING_PLANES), jnp.float32, 0.5, 1.5)
    iteration_total = -rate[None, :] * block_scaling[block_of][:, None] * jitter
    span_offset = jax.random.randint(lane_number[5], (3,), 0, TEXT_SLOTS)
    span_extent = jax.random.uniform(lane_number[6], (3, ASKING_PLANES), jnp.float32, 0.22, 0.69)
    iteration_total = iteration_total.at[span_offset].add(-span_extent)
    return jnp.cumsum(iteration_total, axis=0)


def shard_levels(rng, extent, shards, smallest, largest):
    def one(dim, parts):
        steps = jax.random.uniform(jax.random.fold_in(jax.random.fold_in(rng, 6), dim), (parts,), jnp.float32, smallest / len(shards), largest / len(shards))
        return jnp.repeat(jnp.exp(steps), extent[dim] // parts).reshape((-1,) + (1,) * (len(extent) - dim - 1))

    loudness = one(*shards[0])
    for cut in shards[1:]:
        loudness = loudness * one(*cut)
    return loudness


def profile(amount, total, most, skew):
    portions = [(1 << 20) // math.isqrt(grade ** skew) + 1 for grade in range(2, amount + 1)]
    rest, given = total - most - (amount - 1), [1] * (amount - 1)
    while rest > 0:
        free = [i for i in range(amount - 1) if given[i] < most]
        whole, left = sum([portions[i] for i in free]), rest
        for i in free:
            more = min(most - given[i], max(1, left * portions[i] // whole), rest)
            given[i] = given[i] + more
            rest = rest - more
    return np.array([most] + given)


def uneven(stream_key, count, total, reach, lean):
    if count == 2:
        one = jax.random.randint(stream_key, (), max(1, total - reach), min(reach, total - 1) + 1)
        return jnp.stack([one, total - one])
    sizes = jnp.asarray(profile(count, total, reach, lean), jnp.int32)
    couples = (count - 1) // 2
    giver, receiver = sizes[1:1 + 2 * couples:2], sizes[2:2 + 2 * couples:2]
    slack = jnp.minimum(giver - 1, reach - receiver)
    shifted = jax.random.randint(jax.random.fold_in(stream_key, 1), (couples,), 0, 1 << 20) % (slack + 1)
    sizes = sizes.at[1:1 + 2 * couples:2].set(giver - shifted).at[2:2 + 2 * couples:2].set(receiver + shifted)
    return sizes[jax.random.permutation(jax.random.fold_in(stream_key, 2), count)]


def shared_out(stream_key, own, number, rows, count, top, limit, slope):
    ranking = jax.random.permutation(stream_key, count)
    packed, ordinary = portions_of(count, rows * top, limit, slope, True), portions_of(count, rows * top, limit, slope, False)
    places = jnp.arange(count)

    def named(lengths, offset_by):
        used = int((lengths > 0).sum())
        fixed = max(1, used // 4)
        moved = fixed + (places - fixed + offset_by * (used - fixed)) % max(1, count - fixed)
        return jnp.zeros((count,), jnp.int32).at[ranking[jnp.where(places < fixed, places, moved)]].set(jnp.asarray(lengths, jnp.int32))

    lengths = jnp.where(number % 4 == 0, named(packed, number // 4), named(ordinary, number - number // 4 - 1))
    mixed = jax.random.permutation(jax.random.fold_in(own, 3), count)
    giver, taker = mixed[0:count // 2 * 2:2], mixed[1:count // 2 * 2:2]
    slack = jnp.minimum(lengths[giver] - 1, limit - lengths[taker]) // 2
    slack = jnp.where((giver == ranking[0]) | (taker == ranking[0]) | (lengths[taker] == 0), 0, jnp.maximum(slack, 0))
    moved = jax.random.randint(jax.random.fold_in(own, 4), (count // 2,), 0, 1 << 20) % (slack + 1)
    lengths = lengths.at[giver].add(-moved).at[taker].add(moved)
    members = jnp.searchsorted(jnp.cumsum(lengths), jnp.arange(rows * top), side="right").astype(jnp.int32)
    table = members.reshape(top, rows).T
    table = table[jax.random.permutation(jax.random.fold_in(own, 1), rows)]
    offset_by = jax.random.randint(jax.random.fold_in(own, 2), (rows, 1), 0, top)
    return jnp.take_along_axis(table, (jnp.arange(top)[None, :] + offset_by) % top, axis=1)


def portions_of(number_of, total, most, lean, full):
    portions = [(1 << 20) // math.isqrt(grade ** lean) + 1 for grade in range(1, number_of + 1)]
    largest = most if full else min(most, max(-(-total // number_of), total * portions[0] // sum(portions)))
    least = 1 if total - largest >= number_of - 1 else 0
    counts, spare = [largest] + [least] * (number_of - 1), total - largest - least * (number_of - 1)
    while spare > 0:
        movable = [i for i in range(1, number_of) if counts[i] < largest] or [i for i in range(1, number_of) if counts[i] < most]
        mass, remaining = sum([portions[i] for i in movable]), spare
        for i in movable:
            addition = min(most - counts[i], max(1, remaining * portions[i] // mass), spare)
            counts[i] = counts[i] + addition
            spare = spare - addition
    return np.array(counts)


def centred(key, dims, width, most, cuts=(), kind=jnp.bfloat16):
    values = width * jax.random.normal(key, dims, jnp.float32)
    if cuts:
        values = values * shard_levels(key, dims, cuts, -0.22, 0.18)
    return jnp.clip(values, -most, most).astype(kind)


def setup_inputs(seed: int = 0) -> dict:
    arg_keys = jax.random.split(jax.random.key(seed), 14)
    queries = draw_queries(jax.random.fold_in(arg_keys[13], 71), 0)
    keys = draw_keys(jax.random.fold_in(arg_keys[13], 71), 0)
    values = centred(arg_keys[2], (TEXT_SLOTS, KV_HEADS * HEAD_DIM), 1.0, 6.0, ((0, 8), (1, 4)))
    cum_gate = draw_cum_gate(jax.random.fold_in(arg_keys[13], 71), 0)
    doc_ids = jnp.searchsorted(jnp.cumsum(uneven(arg_keys[4], DOCS, TEXT_SLOTS, DOC_MOST, 0)), jnp.arange(TEXT_SLOTS), side="right").astype(jnp.int32)
    residual = centred(arg_keys[5], (TEXT_SLOTS, D), 1.0, 6.0, ((0, 32),))
    out_proj = centred(arg_keys[6], (ASKING_PLANES * HEAD_DIM, D), (ASKING_PLANES * HEAD_DIM) ** -0.5, 0.1875)
    norm_gain = jnp.clip(1.0 + 0.18 * jax.random.normal(arg_keys[7], (D,), jnp.float32), 0.1, 1.9)
    route_ids_keys = jax.random.split(jax.random.fold_in(arg_keys[8], 1), TEXT_SLOTS // ROWS_DEV)
    route_ids_turns = jax.random.permutation(jax.random.fold_in(arg_keys[8], 3), TEXT_SLOTS // ROWS_DEV)
    route_ids = jax.vmap(lambda own, number: shared_out(jax.random.fold_in(arg_keys[8], 2), own, number, ROWS_DEV, EXPERTS, TOP, CAP, 2))(route_ids_keys, route_ids_turns).reshape((TEXT_SLOTS, TOP))
    route_weights = jnp.clip(jnp.exp(math.log(1.0) - 1.609438 * jax.random.uniform(arg_keys[9], (TEXT_SLOTS, TOP), jnp.float32) ** shard_levels(arg_keys[9], (TEXT_SLOTS, TOP), ((0, 32),), -0.2, 0.2)), 0.2, 1.0)
    expert_gate = centred(arg_keys[10], (EXPERTS, D, EXPERT_FF), D ** -0.5, 0.125, ((0, 8), (2, 4)))
    expert_up = centred(arg_keys[11], (EXPERTS, D, EXPERT_FF), D ** -0.5, 0.125, ((0, 8), (2, 4)))
    expert_down = centred(arg_keys[12], (EXPERTS, EXPERT_FF, D), EXPERT_FF ** -0.5, 0.1875, ((0, 8), (1, 4)))
    return dict(queries=queries, keys=keys, values=values, cum_gate=cum_gate, doc_ids=doc_ids, residual=residual, out_proj=out_proj, norm_gain=norm_gain, route_ids=route_ids, route_weights=route_weights, expert_gate=expert_gate, expert_up=expert_up, expert_down=expert_down)


def head_attention(query_head, key_head, value_head, gate_head, doc_ids):
    qblock = math.gcd(TEXT_SLOTS, 512)
    scale = HEAD_DIM ** (-0.5)
    positions = jnp.arange(TEXT_SLOTS, dtype=jnp.int32)

    def one_block(index):
        first = index * qblock
        query_rows = lax.dynamic_slice_in_dim(query_head, first, qblock, 0)
        gate_rows = lax.dynamic_slice_in_dim(gate_head, first, qblock, 0)
        doc_rows = lax.dynamic_slice_in_dim(doc_ids, first, qblock, 0)
        query_pos = first + jnp.arange(qblock, dtype=jnp.int32)
        scores = jnp.dot(query_rows, key_head.T, preferred_element_type=jnp.float32) * scale
        scores = scores + gate_rows[:, None] - gate_head[None, :]
        allowed = (positions[None, :] <= query_pos[:, None]) & (doc_ids[None, :] == doc_rows[:, None])
        scores = jnp.where(allowed, scores, -jnp.inf)
        top = lax.optimization_barrier(jnp.max(scores, axis=1, keepdims=True))
        expo = jnp.exp(scores - top)
        total = lax.optimization_barrier(jnp.sum(expo, axis=1, keepdims=True))
        summed = jnp.dot(expo.astype(jnp.bfloat16), value_head, preferred_element_type=jnp.float32)
        return (summed / total).astype(jnp.bfloat16)
    blocks = lax.map(one_block, jnp.arange(TEXT_SLOTS // qblock, dtype=jnp.int32))
    return blocks.reshape(TEXT_SLOTS, HEAD_DIM)

def reference(queries, keys, values, cum_gate, doc_ids, residual, out_proj, norm_gain, route_ids, route_weights, expert_gate, expert_up, expert_down):
    group_size = ASKING_PLANES // KV_HEADS
    query_heads = queries.reshape(TEXT_SLOTS, ASKING_PLANES, HEAD_DIM).transpose(1, 0, 2)
    key_heads = keys.reshape(TEXT_SLOTS, KV_HEADS, HEAD_DIM).transpose(1, 0, 2)
    value_heads = values.reshape(TEXT_SLOTS, KV_HEADS, HEAD_DIM).transpose(1, 0, 2)
    gate_heads = cum_gate.T
    owner = jnp.arange(ASKING_PLANES, dtype=jnp.int32) // group_size

    def per_head(inputs):
        query_head, gate_head, kv_index = inputs
        return head_attention(query_head, key_heads[kv_index], value_heads[kv_index], gate_head, doc_ids)
    attended = lax.map(per_head, (query_heads, gate_heads, owner))
    attended = attended.transpose(1, 0, 2).reshape(TEXT_SLOTS, ASKING_PLANES * HEAD_DIM)
    projected = jnp.dot(attended, out_proj, preferred_element_type=jnp.float32)
    stream = (residual.astype(jnp.float32) + projected).astype(jnp.bfloat16)
    stream_f = stream.astype(jnp.float32)
    normed = stream_f * lax.rsqrt(lax.optimization_barrier(jnp.mean(stream_f * stream_f, axis=1, keepdims=True)) + 1e-06)
    normed = (normed * norm_gain[None, :]).astype(jnp.bfloat16)
    block_count = TEXT_SLOTS // ROWS_DEV
    flat = route_ids.reshape(block_count, ROWS_DEV * TOP)
    onehot = (flat[..., None] == jnp.arange(EXPERTS, dtype=jnp.int32)).astype(jnp.int32)
    earlier = jnp.cumsum(onehot, axis=1) - onehot
    rank = lax.optimization_barrier(jnp.sum(earlier * onehot, axis=2))
    per_expert = block_count * CAP
    block_index = jnp.arange(block_count, dtype=jnp.int32)[:, None]
    slot = (flat * per_expert + block_index * CAP + rank).reshape(-1)
    token_of = jnp.arange(TEXT_SLOTS * TOP, dtype=jnp.int32) // TOP
    table = jnp.full((EXPERTS * per_expert,), TEXT_SLOTS, jnp.int32).at[slot].set(token_of)
    weight_table = jnp.zeros((EXPERTS * per_expert,), jnp.float32).at[slot].set(route_weights.reshape(-1))
    padded = jnp.concatenate([normed, jnp.zeros((1, D), jnp.bfloat16)], axis=0)
    quarter = EXPERT_FF // N_TP

    def one_expert(accum, inputs):
        index_rows, weight_rows, gate_weight, up_w, down_w = inputs
        rows = padded[index_rows]
        gate = jnp.dot(rows, gate_weight, preferred_element_type=jnp.float32)
        upper = jnp.dot(rows, up_w, preferred_element_type=jnp.float32)
        hidden = (jax.nn.silu(gate) * upper).astype(jnp.bfloat16)
        hidden_groups = hidden.reshape(per_expert, N_TP, quarter).astype(jnp.float32)
        down_groups = down_w.reshape(N_TP, quarter, D).astype(jnp.float32)
        pieces = jnp.einsum('rgf,gfd->grd', hidden_groups, down_groups).astype(jnp.bfloat16)
        pieces = lax.optimization_barrier(pieces)
        expert_out = lax.optimization_barrier(jnp.sum(pieces.astype(jnp.float32), axis=0)).astype(jnp.bfloat16)
        accum = accum.at[index_rows].add(weight_rows[:, None] * expert_out.astype(jnp.float32))
        return (accum, None)
    accum, _ = lax.scan(one_expert, jnp.zeros((TEXT_SLOTS + 1, D), jnp.float32), (table.reshape(EXPERTS, per_expert), weight_table.reshape(EXPERTS, per_expert), expert_gate, expert_up, expert_down))
    return (stream_f + accum[:TEXT_SLOTS]).astype(jnp.bfloat16)
```

```python
import functools

import jax
import jax.numpy as jnp
from jax import lax
from jax.experimental import pallas as pl
from jax.experimental.pallas import tpu as pltpu
from jax.sharding import PartitionSpec as P

D = 2048
HEAD_DIM = 64
TOP = 2


very_low = -1e30
norm_eps = 1e-06


def slot_ranks(picked_ids, experts):
    onehot = (picked_ids[..., None] == jnp.arange(experts, dtype=jnp.int32)).astype(jnp.int32)
    earlier = jnp.cumsum(onehot, axis=-2) - onehot
    return jnp.sum(earlier * onehot, axis=-1)


def local(
    queries,
    keys,
    values,
    cum_gate,
    doc_ids,
    residual,
    out_proj,
    norm_gain,
    route_ids,
    route_weights,
    expert_gate,
    expert_up,
    expert_down,
):
    own_tokens = queries.shape[0]
    head_count = queries.shape[1] // HEAD_DIM
    kv_count = keys.shape[1] // HEAD_DIM
    group_size = head_count // kv_count
    scale = HEAD_DIM ** (-0.5)
    own_start = lax.axis_index("sp") * own_tokens
    query_pos = own_start + jnp.arange(own_tokens, dtype=jnp.int32)
    query_heads = queries.reshape(own_tokens, kv_count, group_size, HEAD_DIM)
    query_gate = cum_gate.reshape(own_tokens, kv_count, group_size)
    gate_all, doc_all = (
        lax.all_gather(cum_gate, "sp", axis=0, tiled=True),
        lax.all_gather(doc_ids, "sp", axis=0, tiled=True),
    )

    def attend(state, key_block, value_block, first, block_len):
        gate_keys = lax.dynamic_slice_in_dim(gate_all, first, block_len, 0)
        doc_keys = lax.dynamic_slice_in_dim(doc_all, first, block_len, 0)
        key_heads = key_block.reshape(block_len, kv_count, HEAD_DIM)
        value_heads = value_block.reshape(block_len, kv_count, HEAD_DIM)
        scores = (
            jnp.einsum("tkgd,skd->tkgs", query_heads, key_heads, preferred_element_type=jnp.float32)
            * scale
        )
        scores = (
            scores
            + query_gate[..., None]
            - gate_keys.T.reshape(kv_count, group_size, block_len)[None]
        )
        key_pos = first + jnp.arange(block_len, dtype=jnp.int32)
        allowed = (key_pos[None, :] <= query_pos[:, None]) & (doc_keys[None, :] == doc_ids[:, None])
        allowed = allowed[:, None, None, :]
        scores = jnp.where(allowed, scores, very_low)
        top_old, total_old, summed_old = state
        top_new = jnp.maximum(top_old, jnp.max(scores, axis=-1))
        weights = jnp.where(allowed, jnp.exp(scores - top_new[..., None]), 0.0)
        fade = jnp.exp(top_old - top_new)
        total_new = total_old * fade + jnp.sum(weights, axis=-1)
        summed_new = summed_old * fade[..., None] + jnp.einsum(
            "tkgs,skd->tkgd",
            weights.astype(jnp.bfloat16),
            value_heads,
            preferred_element_type=jnp.float32,
        )
        return (top_new, total_new, summed_new)

    start_state = (
        jnp.full((own_tokens, kv_count, group_size), very_low, jnp.float32),
        jnp.zeros((own_tokens, kv_count, group_size), jnp.float32),
        jnp.zeros((own_tokens, kv_count, group_size, HEAD_DIM), jnp.float32),
    )
    key_piece = lax.all_gather(keys, "sp", axis=0, tiled=True)
    value_piece = lax.all_gather(values, "sp", axis=0, tiled=True)
    piece_len = key_piece.shape[0]
    block_len = min(piece_len, own_tokens)

    def one_block(index, inner):
        offset = index * block_len
        key_block = lax.dynamic_slice_in_dim(key_piece, offset, block_len, 0)
        value_block = lax.dynamic_slice_in_dim(value_piece, offset, block_len, 0)
        last_doc = lax.dynamic_index_in_dim(doc_all, offset + block_len - 1, 0, keepdims=False)
        needed = (offset <= own_start + own_tokens - 1) & (last_doc >= doc_ids[0])
        return lax.cond(
            needed,
            lambda carried: attend(carried, key_block, value_block, offset, block_len),
            lambda carried: carried,
            inner,
        )

    top, total, summed = lax.fori_loop(0, piece_len // block_len, one_block, start_state)
    attended = (
        (summed / total[..., None]).reshape(own_tokens, head_count * HEAD_DIM).astype(jnp.bfloat16)
    )
    sp_count = lax.axis_size("sp")
    rows_dev = residual.shape[0]
    plane_entries = lax.all_to_all(attended, "tp", split_axis=0, concat_axis=1, tiled=True)
    projected = jnp.dot(plane_entries, out_proj, preferred_element_type=jnp.float32)
    stream = (residual.astype(jnp.float32) + projected).astype(jnp.bfloat16)
    stream_f = stream.astype(jnp.float32)
    normed = stream_f * lax.rsqrt(jnp.mean(stream_f * stream_f, axis=1, keepdims=True) + norm_eps)
    normed = (normed * norm_gain[None, :]).astype(jnp.bfloat16)
    exp_dev = expert_gate.shape[0]
    experts = exp_dev * sp_count
    capacity = max(2, 2 * rows_dev * TOP // experts)
    own_flat = route_ids.reshape(-1)
    own_rank = slot_ranks(route_ids.reshape(1, rows_dev * TOP), experts)[0]
    own_dest = own_flat * capacity + own_rank
    row_of = jnp.arange(rows_dev * TOP, dtype=jnp.int32) // TOP
    outgoing = jnp.zeros((experts * capacity, D), jnp.bfloat16).at[own_dest].set(normed[row_of])
    arrived = lax.all_to_all(
        outgoing.reshape(experts, capacity, D), "sp", split_axis=0, concat_axis=1, tiled=True
    )
    arrived = arrived.reshape(exp_dev, sp_count, 1, capacity, D)
    piece = lax.all_gather(arrived, "tp", axis=2, tiled=True)
    gate = jnp.einsum("esncd,edf->esncf", piece, expert_gate, preferred_element_type=jnp.float32)
    upper = jnp.einsum("esncd,edf->esncf", piece, expert_up, preferred_element_type=jnp.float32)
    hidden = (jax.nn.silu(gate) * upper).astype(jnp.bfloat16)
    partial_value = jnp.einsum(
        "esncf,efd->esncd", hidden, expert_down, preferred_element_type=jnp.float32
    )
    expert_sums = lax.psum_scatter(
        partial_value.astype(jnp.bfloat16), "tp", scatter_dimension=2, tiled=True
    )
    expert_out = expert_sums.reshape(exp_dev, sp_count * capacity, D)
    returned = lax.all_to_all(expert_out, "sp", split_axis=1, concat_axis=0, tiled=True)
    selected = returned.reshape(experts * capacity, D)[own_dest]
    weighted = selected.astype(jnp.float32).reshape(rows_dev, TOP, D) * route_weights[..., None]
    return (stream_f + jnp.sum(weighted, axis=1)).astype(jnp.bfloat16)


def fused_kernel(
    q, kv, aux, qaux, res, gain, idr, idc, wts, wo_hbm, wg_hbm, wu_hbm, wd_hbm,
    out,
    wo, wg, wu, wd, kvall, auxall, sc, mx, tot, acc, att, gath, proj, outg,
    xin, p0, p1, p2, p3, r1, r3, ysum, ry, zsum, ret,
    wsem, kv_s, kv_r, ax_s, ax_r, at_s, at_r, d_s, d_r, fy_s, fy_r, fp_s, fp_r, fq_s, fq_r,
    c1_s, c1_r, c3_s, c3_r, cy_s, cy_r, cz_s, cz_r,
    *, n_sp, n_tp, cap,
):
    me = lax.axis_index("sp")
    t = lax.axis_index("tp")
    tok, width = q.shape
    heads = width // HEAD_DIM
    rows = res.shape[0]
    depth = res.shape[1]
    slots = n_sp * cap
    flip = lambda k: t + k - 2 * k * (lax.div(t, k) % 2)
    partner = flip(1)
    across = flip(2)
    corner = 3 - t
    f32, bf16 = jnp.float32, jnp.bfloat16

    def remote(src, dst, ss, rs, dev):
        return pltpu.make_async_remote_copy(
            src_ref=src, dst_ref=dst, send_sem=ss, recv_sem=rs,
            device_id=dev, device_id_type=pl.DeviceIdType.MESH,
        )

    def peer_at(k):
        return lax.rem(me + k, n_sp)

    loads = [
        pltpu.make_async_copy(a, b, wsem.at[i])
        for i, (a, b) in enumerate(((wo_hbm, wo), (wg_hbm, wg), (wu_hbm, wu), (wd_hbm, wd)))
    ]
    for c in loads:
        c.start()

    barrier = pltpu.get_barrier_semaphore()

    def greet(k, _):
        pl.semaphore_signal(barrier, inc=1, device_id=(peer_at(k), t), device_id_type=pl.DeviceIdType.MESH)
        return 0

    lax.fori_loop(1, n_sp, greet, 0)
    for other in (partner, across, corner):
        pl.semaphore_signal(barrier, inc=1, device_id=(me, other), device_id_type=pl.DeviceIdType.MESH)
    pl.semaphore_wait(barrier, n_sp - 1 + n_tp - 1)

    def kv_copies(dst_sp, src_sp):
        return (
            remote(kv, kvall.at[src_sp], kv_s.at[dst_sp], kv_r.at[src_sp], (dst_sp, t)),
            remote(aux, auxall.at[src_sp], ax_s.at[dst_sp], ax_r.at[src_sp], (dst_sp, t)),
        )

    def send_kv(k, _):
        for c in kv_copies(k, me):
            c.start()
        return 0

    lax.fori_loop(me + 1, n_sp, send_kv, 0)
    kvall[me] = kv[...]
    auxall[me] = aux[...]

    qpos = lax.broadcasted_iota(jnp.int32, (tok, tok), 0)
    kpos = lax.broadcasted_iota(jnp.int32, (tok, tok), 1)
    qdoc = qaux[:, heads : heads + 1]
    scale = HEAD_DIM ** (-0.5)
    for h in range(heads):
        mx[h] = jnp.full((tok, tok), very_low, f32)
        tot[h] = jnp.zeros((tok, tok), f32)
        acc[h] = jnp.zeros((tok, 2 * HEAD_DIM), f32)

    def first_pass(k, _):
        j = me - k

        @pl.when(k > 0)
        def _():
            for c in kv_copies(j, j):
                c.wait_recv()

        kb = kvall[j][:, :HEAD_DIM]
        ax = auxall[j]
        allowed = (kpos <= qpos + k * tok) & (ax[heads : heads + 1, :] == qdoc)
        for h in range(heads):
            s = lax.dot_general(
                q[:, h * HEAD_DIM : (h + 1) * HEAD_DIM], kb, (((1,), (1,)), ((), ())),
                preferred_element_type=f32,
            )
            s = s * scale + qaux[:, h : h + 1] - ax[h : h + 1, :]
            s = jnp.where(allowed, s, very_low)
            sc[j, h] = s
            mx[h] = jnp.maximum(mx[h], s)
        return 0

    lax.fori_loop(0, me + 1, first_pass, 0)
    for h in range(heads):
        mx[h] = jnp.broadcast_to(jnp.max(mx[h], axis=1, keepdims=True), (tok, tok))

    def second_pass(k, _):
        j = me - k
        vb = kvall[j]
        for h in range(heads):
            e = jnp.exp(sc[j, h] - mx[h])
            tot[h] = tot[h] + e
            acc[h] = acc[h] + jnp.dot(e.astype(bf16), vb, preferred_element_type=f32)
        return 0

    lax.fori_loop(0, me + 1, second_pass, 0)
    pieces = [
        (acc[h][:, HEAD_DIM:] / jnp.sum(tot[h], axis=1, keepdims=True)).astype(bf16)
        for h in range(heads)
    ]
    att[...] = jnp.concatenate(pieces, axis=1)

    def att_copy(to, frm):
        return remote(
            att.at[pl.ds(pl.multiple_of(to * rows, rows), rows), :], gath.at[frm],
            at_s.at[to], at_r.at[frm], (me, to),
        )

    for other in (across, corner, partner):
        att_copy(other, t).start()
    gath[t] = att[pl.ds(pl.multiple_of(t * rows, rows), rows), :]

    srow = lax.broadcasted_iota(jnp.int32, (slots, rows), 0)
    scol = lax.broadcasted_iota(jnp.int32, (slots, rows), 1)
    named = ((idr[0:1, :] == srow // cap) | (idr[1:2, :] == srow // cap)).astype(f32)
    r_a = lax.broadcasted_iota(jnp.int32, (rows, rows), 0)
    r_b = lax.broadcasted_iota(jnp.int32, (rows, rows), 1)
    before = (r_a < r_b).astype(f32)
    rank = jnp.dot(named.astype(bf16), before.astype(bf16), preferred_element_type=f32)
    pick = jnp.where(rank == (srow % cap).astype(f32), named, 0.0).astype(bf16)
    lane = lax.broadcasted_iota(jnp.int32, (rows, slots), 1)
    back = [(idc[:, k : k + 1] == lane // cap).astype(f32) for k in range(TOP)]
    after = (r_b < r_a).astype(bf16)
    rank_t = jnp.dot(after, (back[0] + back[1]).astype(bf16), preferred_element_type=f32)
    back = [jnp.where(rank_t == (lane % cap).astype(f32), b, 0.0).astype(bf16) for b in back]

    loads[0].wait()
    for i, src in enumerate((t, partner, across, corner)):
        if i:
            att_copy(src, src).wait_recv()
        part = jnp.dot(
            gath[src], wo[pl.ds(pl.multiple_of(src * width, width), width), :],
            preferred_element_type=f32,
        )
        proj[...] = part if i == 0 else proj[...] + part
    stream = (res[...].astype(f32) + proj[...]).astype(bf16)
    stream_f = stream.astype(f32)
    proj[...] = stream_f
    normed = stream_f * lax.rsqrt(jnp.mean(stream_f * stream_f, axis=1, keepdims=True) + norm_eps)
    normed = (normed * gain[...]).astype(bf16)
    outg[...] = (
        jnp.dot(pick, normed, preferred_element_type=f32).astype(bf16).reshape(n_sp, cap, depth)
    )

    def out_copy(to, frm):
        return remote(outg.at[to], xin.at[t, frm], d_s.at[to], d_r.at[frm], (to, t))

    def send_out(k, _):
        out_copy(peer_at(k), me).start()
        return 0

    lax.fori_loop(1, n_sp, send_out, 0)
    xin[t, me] = outg[me]

    def to_across(j, line):
        return remote(xin.at[line, j], xin.at[line, j], fy_s.at[j], fy_r.at[j], (me, across))

    def to_partner(j, line):
        return remote(xin.at[line, j], xin.at[line, j], fp_s.at[j], fp_r.at[j], (me, partner))

    def relay_partner(j, line):
        return remote(xin.at[line, j], xin.at[line, j], fq_s.at[j], fq_r.at[j], (me, partner))

    def source_at(k):
        return lax.rem(me - k + n_sp, n_sp)

    def forward(k, _):
        j = source_at(k)

        @pl.when(k > 0)
        def _():
            out_copy(j, j).wait_recv()

        to_across(j, t).start()
        to_partner(j, t).start()

        @pl.when(k > 0)
        def _():
            i = source_at(k - 1)
            to_across(i, across).wait_recv()
            relay_partner(i, across).start()

        return 0

    lax.fori_loop(0, n_sp, forward, 0)
    last = source_at(n_sp - 1)
    for c in loads[1:]:
        c.wait()

    def expert(line, dst):
        x = xin[line].reshape(slots, depth)
        g = jnp.dot(x, wg[...], preferred_element_type=f32)
        u = jnp.dot(x, wu[...], preferred_element_type=f32)
        hid = (g / (1.0 + jnp.exp(-g)) * u).astype(bf16)
        dst[...] = (
            jnp.dot(hid, wd[...], preferred_element_type=f32).astype(bf16).reshape(n_sp, cap, depth)
        )

    def all_of(fn):
        def body(j, _):
            fn(j)
            return 0

        lax.fori_loop(0, n_sp, body, 0)

    expert(t, p0)
    to_across(last, across).wait_recv()
    relay_partner(last, across).start()
    all_of(lambda j: to_partner(j, partner).wait_recv())
    expert(partner, p1)

    def c1_copy(j):
        return remote(p1.at[j], r1.at[j], c1_s.at[j], c1_r.at[j], (me, partner))

    def c3_copy(j):
        return remote(p3.at[j], r3.at[j], c3_s.at[j], c3_r.at[j], (me, partner))

    def cy_copy(j):
        return remote(ysum.at[j], ry.at[j], cy_s.at[j], cy_r.at[j], (me, across))

    def cz_copy(to, frm):
        return remote(zsum.at[to], ret.at[frm], cz_s.at[to], cz_r.at[frm], (to, t))

    all_of(lambda j: c1_copy(j).start())
    expert(across, p2)
    all_of(lambda j: relay_partner(j, corner).wait_recv())
    expert(corner, p3)

    def order(k):
        return lax.rem(me + k, n_sp)

    def start3(k, _):
        c3_copy(order(k)).start()
        return 0

    lax.fori_loop(1, n_sp + 1, start3, 0)

    def pair_sum(k, _):
        j = order(k)
        c3_copy(j).wait_recv()
        ysum[j] = (p2[j].astype(f32) + r3[j].astype(f32)).astype(bf16)
        cy_copy(j).start()
        return 0

    lax.fori_loop(1, n_sp + 1, pair_sum, 0)

    def full_sum(k, _):
        j = order(k)
        c1_copy(j).wait_recv()
        cy_copy(j).wait_recv()
        zsum[j] = (p0[j].astype(f32) + r1[j].astype(f32) + ry[j].astype(f32)).astype(bf16)

        @pl.when(k < n_sp)
        def _():
            cz_copy(j, me).start()

        return 0

    lax.fori_loop(1, n_sp + 1, full_sum, 0)
    ret[me] = zsum[me]

    def wait_ret(k, _):
        j = source_at(k)
        cz_copy(j, j).wait_recv()
        return 0

    lax.fori_loop(1, n_sp, wait_ret, 0)
    total = proj[...]
    got = ret[...].reshape(slots, depth)
    mix = wts[:, 0:1] * jnp.dot(back[0], got, preferred_element_type=f32)
    for k in range(1, TOP):
        mix = mix + wts[:, k : k + 1] * jnp.dot(back[k], got, preferred_element_type=f32)
    out[...] = (total + mix).astype(bf16)

    def end_kv(k, _):
        for c in kv_copies(k, me):
            c.wait_send()
        return 0

    lax.fori_loop(me + 1, n_sp, end_kv, 0)
    for other in (across, corner, partner):
        att_copy(other, t).wait_send()

    def end_peers(k, _):
        j = peer_at(k)
        out_copy(j, me).wait_send()
        cz_copy(j, me).wait_send()
        return 0

    lax.fori_loop(1, n_sp, end_peers, 0)

    def end_all(j):
        to_across(j, t).wait_send()
        to_partner(j, t).wait_send()
        relay_partner(j, across).wait_send()
        c1_copy(j).wait_send()
        c3_copy(j).wait_send()
        cy_copy(j).wait_send()

    all_of(end_all)


def fused(
    queries, keys, values, cum_gate, doc_ids, residual, out_proj, norm_gain,
    route_ids, route_weights, expert_gate, expert_up, expert_down,
):
    n_sp, n_tp = lax.axis_size("sp"), lax.axis_size("tp")
    tok, width = queries.shape
    heads = width // HEAD_DIM
    rows, depth = residual.shape
    cap = max(2, 2 * rows * TOP // n_sp)
    ff = expert_gate.shape[2]
    slots = n_sp * cap
    f32, bf16 = jnp.float32, jnp.bfloat16
    kv = jnp.concatenate([keys, values], axis=1)
    qaux = jnp.concatenate([cum_gate, doc_ids.astype(f32)[:, None]], axis=1)
    height = -(-(heads + 1) // 8) * 8
    aux = jnp.pad(qaux.T, ((0, height - heads - 1), (0, 0)))
    vm = pl.BlockSpec(memory_space=pltpu.VMEM)
    hb = pl.BlockSpec(memory_space=pl.ANY)
    block = pltpu.VMEM((n_sp, cap, depth), bf16)
    dma = lambda n: pltpu.SemaphoreType.DMA((n,))
    call = pl.pallas_call(
        functools.partial(fused_kernel, n_sp=n_sp, n_tp=n_tp, cap=cap),
        out_shape=jax.ShapeDtypeStruct((rows, depth), bf16),
        in_specs=[vm] * 9 + [hb] * 4,
        out_specs=vm,
        scratch_shapes=[
            pltpu.VMEM(out_proj.shape, bf16),
            pltpu.VMEM((depth, ff), bf16),
            pltpu.VMEM((depth, ff), bf16),
            pltpu.VMEM((ff, depth), bf16),
            pltpu.VMEM((n_sp, tok, 2 * HEAD_DIM), bf16),
            pltpu.VMEM((n_sp, height, tok), f32),
            pltpu.VMEM((n_sp, heads, tok, tok), f32),
            pltpu.VMEM((heads, tok, tok), f32),
            pltpu.VMEM((heads, tok, tok), f32),
            pltpu.VMEM((heads, tok, 2 * HEAD_DIM), f32),
            pltpu.VMEM((tok, width), bf16),
            pltpu.VMEM((n_tp, rows, width), bf16),
            pltpu.VMEM((rows, depth), f32),
            block,
            pltpu.VMEM((n_tp, n_sp, cap, depth), bf16),
        ]
        + [block] * 10
        + [dma(4)]
        + [dma(n_sp)] * 4
        + [dma(n_tp)] * 2
        + [dma(n_sp)] * 16,
        compiler_params=pltpu.CompilerParams(
            collective_id=0, has_side_effects=True, vmem_limit_bytes=60 * 1024 * 1024
        ),
    )
    return call(
        queries, kv, aux, qaux, residual, norm_gain.reshape(1, depth),
        route_ids.T, route_ids, route_weights, out_proj, expert_gate[0], expert_up[0], expert_down[0],
    )


def chosen(*args):
    n_sp, n_tp = lax.axis_size("sp"), lax.axis_size("tp")
    queries, keys, residual, expert_gate = args[0], args[1], args[5], args[10]
    cap = max(2, 2 * residual.shape[0] * TOP // n_sp)
    fits = (
        n_tp == 4
        and expert_gate.shape[0] == 1
        and keys.shape[1] == HEAD_DIM
        and queries.shape[0] == 128
        and cap % 16 == 0
        and residual.shape[0] % 32 == 0
    )
    return fused(*args) if fits else local(*args)


def solution(mesh):
    in_specs = (
        P("sp", "tp"),
        P("sp", "tp"),
        P("sp", "tp"),
        P("sp", "tp"),
        P("sp"),
        P(("sp", "tp"), None),
        P(),
        P(),
        P(("sp", "tp"), None),
        P(("sp", "tp"), None),
        P("sp", None, "tp"),
        P("sp", None, "tp"),
        P("sp", "tp", None),
    )
    out_specs = P(("sp", "tp"), None)
    return jax.shard_map(chosen, mesh=mesh, in_specs=in_specs, out_specs=out_specs, check_vma=False)
```

```python
import functools

import jax
import jax.numpy as jnp
from jax import lax
from jax.experimental import pallas as pl
from jax.experimental.pallas import tpu as pltpu
from jax.sharding import PartitionSpec as P

D = 2048
HEAD_DIM = 64
TOP = 2


very_low = -1e30
norm_eps = 1e-06


def slot_ranks(picked_ids, experts):
    onehot = (picked_ids[..., None] == jnp.arange(experts, dtype=jnp.int32)).astype(jnp.int32)
    earlier = jnp.cumsum(onehot, axis=-2) - onehot
    return jnp.sum(earlier * onehot, axis=-1)


def local(
    queries,
    keys,
    values,
    cum_gate,
    doc_ids,
    residual,
    out_proj,
    norm_gain,
    route_ids,
    route_weights,
    expert_gate,
    expert_up,
    expert_down,
):
    own_tokens = queries.shape[0]
    head_count = queries.shape[1] // HEAD_DIM
    kv_count = keys.shape[1] // HEAD_DIM
    group_size = head_count // kv_count
    scale = HEAD_DIM ** (-0.5)
    own_start = lax.axis_index("sp") * own_tokens
    query_pos = own_start + jnp.arange(own_tokens, dtype=jnp.int32)
    query_heads = queries.reshape(own_tokens, kv_count, group_size, HEAD_DIM)
    query_gate = cum_gate.reshape(own_tokens, kv_count, group_size)
    gate_all, doc_all = (
        lax.all_gather(cum_gate, "sp", axis=0, tiled=True),
        lax.all_gather(doc_ids, "sp", axis=0, tiled=True),
    )

    def attend(state, key_block, value_block, first, block_len):
        gate_keys = lax.dynamic_slice_in_dim(gate_all, first, block_len, 0)
        doc_keys = lax.dynamic_slice_in_dim(doc_all, first, block_len, 0)
        key_heads = key_block.reshape(block_len, kv_count, HEAD_DIM)
        value_heads = value_block.reshape(block_len, kv_count, HEAD_DIM)
        scores = (
            jnp.einsum("tkgd,skd->tkgs", query_heads, key_heads, preferred_element_type=jnp.float32)
            * scale
        )
        scores = (
            scores
            + query_gate[..., None]
            - gate_keys.T.reshape(kv_count, group_size, block_len)[None]
        )
        key_pos = first + jnp.arange(block_len, dtype=jnp.int32)
        allowed = (key_pos[None, :] <= query_pos[:, None]) & (doc_keys[None, :] == doc_ids[:, None])
        allowed = allowed[:, None, None, :]
        scores = jnp.where(allowed, scores, very_low)
        top_old, total_old, summed_old = state
        top_new = jnp.maximum(top_old, jnp.max(scores, axis=-1))
        weights = jnp.where(allowed, jnp.exp(scores - top_new[..., None]), 0.0)
        fade = jnp.exp(top_old - top_new)
        total_new = total_old * fade + jnp.sum(weights, axis=-1)
        summed_new = summed_old * fade[..., None] + jnp.einsum(
            "tkgs,skd->tkgd",
            weights.astype(jnp.bfloat16),
            value_heads,
            preferred_element_type=jnp.float32,
        )
        return (top_new, total_new, summed_new)

    start_state = (
        jnp.full((own_tokens, kv_count, group_size), very_low, jnp.float32),
        jnp.zeros((own_tokens, kv_count, group_size), jnp.float32),
        jnp.zeros((own_tokens, kv_count, group_size, HEAD_DIM), jnp.float32),
    )
    key_piece = lax.all_gather(keys, "sp", axis=0, tiled=True)
    value_piece = lax.all_gather(values, "sp", axis=0, tiled=True)
    piece_len = key_piece.shape[0]
    block_len = min(piece_len, own_tokens)

    def one_block(index, inner):
        offset = index * block_len
        key_block = lax.dynamic_slice_in_dim(key_piece, offset, block_len, 0)
        value_block = lax.dynamic_slice_in_dim(value_piece, offset, block_len, 0)
        last_doc = lax.dynamic_index_in_dim(doc_all, offset + block_len - 1, 0, keepdims=False)
        needed = (offset <= own_start + own_tokens - 1) & (last_doc >= doc_ids[0])
        return lax.cond(
            needed,
            lambda carried: attend(carried, key_block, value_block, offset, block_len),
            lambda carried: carried,
            inner,
        )

    top, total, summed = lax.fori_loop(0, piece_len // block_len, one_block, start_state)
    attended = (
        (summed / total[..., None]).reshape(own_tokens, head_count * HEAD_DIM).astype(jnp.bfloat16)
    )
    sp_count = lax.axis_size("sp")
    rows_dev = residual.shape[0]
    plane_entries = lax.all_to_all(attended, "tp", split_axis=0, concat_axis=1, tiled=True)
    projected = jnp.dot(plane_entries, out_proj, preferred_element_type=jnp.float32)
    stream = (residual.astype(jnp.float32) + projected).astype(jnp.bfloat16)
    stream_f = stream.astype(jnp.float32)
    normed = stream_f * lax.rsqrt(jnp.mean(stream_f * stream_f, axis=1, keepdims=True) + norm_eps)
    normed = (normed * norm_gain[None, :]).astype(jnp.bfloat16)
    exp_dev = expert_gate.shape[0]
    experts = exp_dev * sp_count
    capacity = max(2, 2 * rows_dev * TOP // experts)
    own_flat = route_ids.reshape(-1)
    own_rank = slot_ranks(route_ids.reshape(1, rows_dev * TOP), experts)[0]
    own_dest = own_flat * capacity + own_rank
    row_of = jnp.arange(rows_dev * TOP, dtype=jnp.int32) // TOP
    outgoing = jnp.zeros((experts * capacity, D), jnp.bfloat16).at[own_dest].set(normed[row_of])
    arrived = lax.all_to_all(
        outgoing.reshape(experts, capacity, D), "sp", split_axis=0, concat_axis=1, tiled=True
    )
    arrived = arrived.reshape(exp_dev, sp_count, 1, capacity, D)
    piece = lax.all_gather(arrived, "tp", axis=2, tiled=True)
    gate = jnp.einsum("esncd,edf->esncf", piece, expert_gate, preferred_element_type=jnp.float32)
    upper = jnp.einsum("esncd,edf->esncf", piece, expert_up, preferred_element_type=jnp.float32)
    hidden = (jax.nn.silu(gate) * upper).astype(jnp.bfloat16)
    partial_value = jnp.einsum(
        "esncf,efd->esncd", hidden, expert_down, preferred_element_type=jnp.float32
    )
    expert_sums = lax.psum_scatter(
        partial_value.astype(jnp.bfloat16), "tp", scatter_dimension=2, tiled=True
    )
    expert_out = expert_sums.reshape(exp_dev, sp_count * capacity, D)
    returned = lax.all_to_all(expert_out, "sp", split_axis=1, concat_axis=0, tiled=True)
    selected = returned.reshape(experts * capacity, D)[own_dest]
    weighted = selected.astype(jnp.float32).reshape(rows_dev, TOP, D) * route_weights[..., None]
    return (stream_f + jnp.sum(weighted, axis=1)).astype(jnp.bfloat16)


def fused_kernel(
    q, kt, vt, gt, doc, res, gain, idt, wtt, wo_hbm, wg_hbm, wu_hbm, wd_hbm,
    base, mixed,
    wo, wg, wu, wd, qs, kvall, auxall, sc, mx, tot, acc, att, gath, proj, outg,
    xin, p0, p1, p2, p3, r1, r3, ysum, ry, zsum, ret,
    wsem, kv_s, kv_r, ax_s, ax_r, kq_s, aq_s, at_s, at_r, d_s, d_r, fy_s, fy_r, fp_s, fp_r, fq_s, fq_r,
    c1_s, c1_r, c3_s, c3_r, cy_s, cy_r, cz_s, cz_r,
    *, n_sp, n_tp, cap,
):
    me = lax.axis_index("sp")
    t = lax.axis_index("tp")
    tok, width = q.shape
    heads = width // HEAD_DIM
    rows = res.shape[0]
    depth = res.shape[1]
    slots = n_sp * cap
    half = n_sp // 2
    flip = lambda k: t + k - 2 * k * (lax.div(t, k) % 2)
    partner = flip(1)
    across = flip(2)
    corner = 3 - t
    sib = me + 1 - 2 * lax.rem(me, 2)
    f32, bf16 = jnp.float32, jnp.bfloat16

    def remote(src, dst, ss, rs, dev):
        return pltpu.make_async_remote_copy(
            src_ref=src, dst_ref=dst, send_sem=ss, recv_sem=rs,
            device_id=dev, device_id_type=pl.DeviceIdType.MESH,
        )

    def peer_at(k):
        return lax.rem(me + k, n_sp)

    def source_at(k):
        return lax.rem(me - k + n_sp, n_sp)

    def span(lo, hi, fn):
        def body(k, _):
            fn(k)
            return 0

        lax.fori_loop(lo, hi, body, 0)

    loads = [
        pltpu.make_async_copy(a, b, wsem.at[i])
        for i, (a, b) in enumerate(((wo_hbm, wo), (wg_hbm, wg), (wu_hbm, wu), (wd_hbm, wd)))
    ]
    for c in loads:
        c.start()
    kvall[me, :HEAD_DIM, :] = kt[...]
    kvall[me, HEAD_DIM:, :] = vt[...]
    auxall[me, :heads, :] = gt[...]
    auxall[me, heads : heads + 1, :] = doc[...].astype(f32)

    barrier = pltpu.get_barrier_semaphore()
    span(1, n_sp, lambda k: pl.semaphore_signal(
        barrier, inc=1, device_id=(peer_at(k), t), device_id_type=pl.DeviceIdType.MESH))
    for other in (partner, across, corner):
        pl.semaphore_signal(barrier, inc=1, device_id=(me, other), device_id_type=pl.DeviceIdType.MESH)

    def column(row, size):
        eye = lax.broadcasted_iota(jnp.int32, (size, size), 0) == lax.broadcasted_iota(
            jnp.int32, (size, size), 1
        )
        return jnp.sum(jnp.where(eye, jnp.broadcast_to(row, (size, size)), 0.0), axis=1, keepdims=True)

    qpos = lax.broadcasted_iota(jnp.int32, (tok, tok), 0)
    kpos = lax.broadcasted_iota(jnp.int32, (tok, tok), 1)
    qdoc = column(doc[...].astype(f32), tok)
    qgate = [column(gt[h : h + 1, :], tok) for h in range(heads)]
    scale = HEAD_DIM ** (-0.5)
    for h in range(heads):
        qs[h] = q[:, h * HEAD_DIM : (h + 1) * HEAD_DIM]
        mx[h] = jnp.full((tok, tok), very_low, f32)
        tot[h] = jnp.zeros((tok, tok), f32)
        acc[h] = jnp.zeros((tok, HEAD_DIM), f32)
    pl.semaphore_wait(barrier, n_sp - 1 + n_tp - 1)
    def kv_copies(to, frm):
        return (
            remote(kvall.at[frm], kvall.at[frm], kv_s.at[to], kv_r.at[frm], (to, t)),
            remote(auxall.at[frm], auxall.at[frm], ax_s.at[to], ax_r.at[frm], (to, t)),
        )

    def kv_relays(frm):
        return (
            remote(kvall.at[frm], kvall.at[frm], kq_s.at[frm], kv_r.at[frm], (sib, t)),
            remote(auxall.at[frm], auxall.at[frm], aq_s.at[frm], ax_r.at[frm], (sib, t)),
        )

    ahead = lax.div(n_sp - 1 - me, 2)

    def kv_out(do):
        def one(m):
            for c in kv_copies(me + 2 * (ahead - m), me):
                do(c)

        span(0, ahead, one)

        @pl.when(sib > me)
        def _():
            for c in kv_copies(sib, me):
                do(c)

    kv_out(lambda c: c.start())

    def score_block(j):
        kb = kvall[j, :HEAD_DIM, :]
        ax = auxall[j]
        allowed = (kpos + j * tok <= qpos + me * tok) & (ax[heads : heads + 1, :] == qdoc)
        for h in range(heads):
            s = jnp.dot(qs[h], kb, preferred_element_type=f32)
            s = s * scale + qgate[h] - ax[h : h + 1, :]
            s = jnp.where(allowed, s, very_low)
            sc[j, h] = s
            mx[h] = jnp.maximum(mx[h], s)

    score_block(me)

    def same_parity(m):
        j = me - 2 * m
        for c in kv_copies(j, j):
            c.wait_recv()
        for c in kv_relays(j):
            c.start()
        score_block(j)

    span(1, lax.div(me, 2) + 1, same_parity)

    def other_parity(m):
        j = me - 1 - 2 * m
        for c in kv_copies(j, j):
            c.wait_recv()
        score_block(j)

    span(0, lax.div(me + 1, 2), other_parity)
    for h in range(heads):
        mx[h] = jnp.broadcast_to(jnp.max(mx[h], axis=1, keepdims=True), (tok, tok))

    def second_pass(j):
        vb = kvall[j, HEAD_DIM:, :]
        for h in range(heads):
            e = jnp.exp(sc[j, h] - mx[h])
            tot[h] = tot[h] + e
            acc[h] = acc[h] + lax.dot_general(
                e.astype(bf16), vb, (((1,), (1,)), ((), ())), preferred_element_type=f32
            )

    span(0, me + 1, second_pass)
    pieces = [
        (acc[h] / jnp.sum(tot[h], axis=1, keepdims=True)).astype(bf16) for h in range(heads)
    ]
    att[...] = jnp.concatenate(pieces, axis=1)
    def att_copy(to, frm):
        return remote(
            att.at[pl.ds(pl.multiple_of(to * rows, rows), rows), :], gath.at[frm],
            at_s.at[to], at_r.at[frm], (me, to),
        )

    for other in (across, corner, partner):
        att_copy(other, t).start()
    gath[t] = att[pl.ds(pl.multiple_of(t * rows, rows), rows), :]

    srow = lax.broadcasted_iota(jnp.int32, (slots, rows), 0)
    named = ((idt[0:1, :] == srow // cap) | (idt[1:2, :] == srow // cap)).astype(f32)
    r_a = lax.broadcasted_iota(jnp.int32, (rows, rows), 0)
    r_b = lax.broadcasted_iota(jnp.int32, (rows, rows), 1)
    before = (r_a < r_b).astype(bf16)
    rank = jnp.dot(named.astype(bf16), before, preferred_element_type=f32)
    pick = jnp.where(rank == (srow % cap).astype(f32), named, 0.0).astype(bf16)
    lane = lax.broadcasted_iota(jnp.int32, (rows, slots), 1)
    owner = (lane // cap).astype(f32)
    back = [(column(idt[k : k + 1, :].astype(f32), rows) == owner).astype(f32) for k in range(TOP)]
    share = [column(wtt[k : k + 1, :], rows) for k in range(TOP)]
    after = (r_b < r_a).astype(bf16)
    rank_t = jnp.dot(after, (back[0] + back[1]).astype(bf16), preferred_element_type=f32)
    back = [jnp.where(rank_t == (lane % cap).astype(f32), b, 0.0).astype(bf16) for b in back]
    loads[0].wait()
    for i, src in enumerate((t, partner, across, corner)):
        if i:
            att_copy(src, src).wait_recv()
        part = jnp.dot(
            gath[src], wo[pl.ds(pl.multiple_of(src * width, width), width), :],
            preferred_element_type=f32,
        )
        proj[...] = part if i == 0 else proj[...] + part
    stream = (res[...].astype(f32) + proj[...]).astype(bf16)
    base[...] = stream
    stream_f = stream.astype(f32)
    normed = stream_f * lax.rsqrt(jnp.mean(stream_f * stream_f, axis=1, keepdims=True) + norm_eps)
    normed = (normed * gain[...]).astype(bf16)
    outg[...] = (
        jnp.dot(pick, normed, preferred_element_type=f32).astype(bf16).reshape(n_sp, cap, depth)
    )
    def out_copy(k):
        to = peer_at(k)
        return remote(outg.at[to], xin.at[t, k], d_s.at[k], d_r.at[k], (to, t))

    def to_across(k, line):
        return remote(xin.at[line, k], xin.at[line, k], fy_s.at[k], fy_r.at[k], (me, across))

    def to_partner(k, line):
        return remote(xin.at[line, k], xin.at[line, k], fp_s.at[k], fp_r.at[k], (me, partner))

    def relay_partner(k, line):
        return remote(xin.at[line, k], xin.at[line, k], fq_s.at[k], fq_r.at[k], (me, partner))

    def c1_copy(k):
        return remote(p1.at[k], r1.at[k], c1_s.at[k], c1_r.at[k], (me, partner))

    def c3_copy(k):
        return remote(p3.at[k], r3.at[k], c3_s.at[k], c3_r.at[k], (me, partner))

    def cy_copy(k):
        return remote(ysum.at[k], ry.at[k], cy_s.at[k], cy_r.at[k], (me, across))

    def cz_copy(k, frm):
        return remote(zsum.at[k], ret.at[frm], cz_s.at[k], cz_r.at[k], (source_at(k), t))

    span(1, n_sp, lambda k: out_copy(k).start())
    xin[t, 0] = outg[me]
    to_across(0, t).start()
    to_partner(0, t).start()

    def relay(k):
        to_across(k, across).wait_recv()
        relay_partner(k, across).start()

    def forward(k):
        out_copy(k).wait_recv()
        to_across(k, t).start()
        to_partner(k, t).start()
        relay(k - 1)

    def expert(line, lo, dst):
        x = xin[line, lo : lo + half].reshape(half * cap, depth)
        g = jnp.dot(x, wg[...], preferred_element_type=f32)
        u = jnp.dot(x, wu[...], preferred_element_type=f32)
        hid = (g / (1.0 + jnp.exp(-g)) * u).astype(bf16)
        dst[lo : lo + half] = (
            jnp.dot(hid, wd[...], preferred_element_type=f32).astype(bf16).reshape(half, cap, depth)
        )

    def pair_sum(k):
        c3_copy(k).wait_recv()
        ysum[k] = (p2[k].astype(f32) + r3[k].astype(f32)).astype(bf16)
        cy_copy(k).start()

    def full_sum(k):
        c1_copy(k).wait_recv()
        cy_copy(k).wait_recv()
        zsum[k] = (p0[k].astype(f32) + r1[k].astype(f32) + ry[k].astype(f32)).astype(bf16)

        @pl.when(k > 0)
        def _():
            cz_copy(k, me).start()

    span(1, half + 1, forward)
    for c in loads[1:]:
        c.wait()
    expert(t, 0, p0)
    span(half + 1, half + 2, forward)
    span(0, half, lambda k: to_partner(k, partner).wait_recv())
    expert(partner, 0, p1)
    span(0, half, lambda k: c1_copy(k).start())
    span(half + 2, n_sp - 1, forward)
    span(0, half, lambda k: relay_partner(k, corner).wait_recv())
    expert(corner, 0, p3)
    span(0, half, lambda k: c3_copy(k).start())
    span(n_sp - 1, n_sp, forward)
    expert(across, 0, p2)
    span(0, half, pair_sum)
    expert(t, half, p0)
    relay(n_sp - 1)
    span(half, n_sp, lambda k: to_partner(k, partner).wait_recv())
    expert(partner, half, p1)
    span(half, n_sp, lambda k: c1_copy(k).start())
    span(half, n_sp, lambda k: relay_partner(k, corner).wait_recv())
    expert(corner, half, p3)
    span(half, n_sp, lambda k: c3_copy(k).start())
    expert(across, half, p2)
    span(half, n_sp, pair_sum)
    span(0, half, full_sum)
    span(half, n_sp, full_sum)
    ret[me] = zsum[0]
    span(1, n_sp, lambda k: cz_copy(k, peer_at(k)).wait_recv())
    got = ret[...].reshape(slots, depth)
    mix = share[0] * jnp.dot(back[0], got, preferred_element_type=f32)
    for k in range(1, TOP):
        mix = mix + share[k] * jnp.dot(back[k], got, preferred_element_type=f32)
    mixed[...] = mix
    kv_out(lambda c: c.wait_send())

    def end_relay(m):
        for c in kv_relays(me - 2 * m):
            c.wait_send()

    span(1, lax.div(me, 2) + 1, end_relay)
    for other in (across, corner, partner):
        att_copy(other, t).wait_send()

    def end_peers(k):
        out_copy(k).wait_send()
        cz_copy(k, me).wait_send()

    span(1, n_sp, end_peers)

    def end_all(k):
        to_across(k, t).wait_send()
        to_partner(k, t).wait_send()
        relay_partner(k, across).wait_send()
        c1_copy(k).wait_send()
        c3_copy(k).wait_send()
        cy_copy(k).wait_send()

    span(0, n_sp, end_all)


def fused(
    queries, keys, values, cum_gate, doc_ids, residual, out_proj, norm_gain,
    route_ids, route_weights, expert_gate, expert_up, expert_down,
):
    n_sp, n_tp = lax.axis_size("sp"), lax.axis_size("tp")
    tok, width = queries.shape
    heads = width // HEAD_DIM
    rows, depth = residual.shape
    cap = max(2, 2 * rows * TOP // n_sp)
    ff = expert_gate.shape[2]
    slots = n_sp * cap
    f32, bf16 = jnp.float32, jnp.bfloat16
    height = -(-(heads + 1) // 8) * 8
    vm = pl.BlockSpec(memory_space=pltpu.VMEM)
    hb = pl.BlockSpec(memory_space=pl.ANY)
    block = pltpu.VMEM((n_sp, cap, depth), bf16)
    dma = lambda n: pltpu.SemaphoreType.DMA((n,))
    call = pl.pallas_call(
        functools.partial(fused_kernel, n_sp=n_sp, n_tp=n_tp, cap=cap),
        out_shape=(
            jax.ShapeDtypeStruct((rows, depth), bf16),
            jax.ShapeDtypeStruct((rows, depth), f32),
        ),
        in_specs=[vm] * 9 + [hb] * 4,
        out_specs=(vm, vm),
        scratch_shapes=[
            pltpu.VMEM(out_proj.shape, bf16),
            pltpu.VMEM((depth, ff), bf16),
            pltpu.VMEM((depth, ff), bf16),
            pltpu.VMEM((ff, depth), bf16),
            pltpu.VMEM((heads, tok, HEAD_DIM), bf16),
            pltpu.VMEM((n_sp, 2 * HEAD_DIM, tok), bf16),
            pltpu.VMEM((n_sp, height, tok), f32),
            pltpu.VMEM((n_sp, heads, tok, tok), f32),
            pltpu.VMEM((heads, tok, tok), f32),
            pltpu.VMEM((heads, tok, tok), f32),
            pltpu.VMEM((heads, tok, HEAD_DIM), f32),
            pltpu.VMEM((tok, width), bf16),
            pltpu.VMEM((n_tp, rows, width), bf16),
            pltpu.VMEM((rows, depth), f32),
            block,
            pltpu.VMEM((n_tp, n_sp, cap, depth), bf16),
        ]
        + [block] * 10
        + [dma(4)]
        + [dma(n_sp)] * 6
        + [dma(n_tp)] * 2
        + [dma(n_sp)] * 16,
        compiler_params=pltpu.CompilerParams(
            collective_id=0, has_side_effects=True, vmem_limit_bytes=60 * 1024 * 1024
        ),
    )
    base, mixed = call(
        queries, keys.T, values.T, cum_gate.T, doc_ids.reshape(1, tok), residual, norm_gain.reshape(1, depth),
        route_ids.T, route_weights.T, out_proj, expert_gate[0], expert_up[0], expert_down[0],
    )
    return (base.astype(f32) + mixed).astype(bf16)


def chosen(*args):
    n_sp, n_tp = lax.axis_size("sp"), lax.axis_size("tp")
    queries, keys, residual, expert_gate = args[0], args[1], args[5], args[10]
    cap = max(2, 2 * residual.shape[0] * TOP // n_sp)
    fits = (
        n_tp == 4
        and n_sp % 2 == 0
        and n_sp >= 8
        and expert_gate.shape[0] == 1
        and keys.shape[1] == HEAD_DIM
        and queries.shape[0] == 128
        and cap % 16 == 0
        and residual.shape[0] % 32 == 0
    )
    return fused(*args) if fits else local(*args)


def solution(mesh):
    in_specs = (
        P("sp", "tp"),
        P("sp", "tp"),
        P("sp", "tp"),
        P("sp", "tp"),
        P("sp"),
        P(("sp", "tp"), None),
        P(),
        P(),
        P(("sp", "tp"), None),
        P(("sp", "tp"), None),
        P("sp", None, "tp"),
        P("sp", None, "tp"),
        P("sp", "tp", None),
    )
    out_specs = P(("sp", "tp"), None)
    return jax.shard_map(chosen, mesh=mesh, in_specs=in_specs, out_specs=out_specs, check_vma=False)
```

```python
import functools

import jax
import jax.numpy as jnp
from jax import lax
from jax.experimental import pallas as pl
from jax.experimental.pallas import tpu as pltpu
from jax.sharding import PartitionSpec as P

D = 2048
HEAD_DIM = 64
TOP = 2


very_low = -1e30
norm_eps = 1e-06


def slot_ranks(picked_ids, experts):
    onehot = (picked_ids[..., None] == jnp.arange(experts, dtype=jnp.int32)).astype(jnp.int32)
    earlier = jnp.cumsum(onehot, axis=-2) - onehot
    return jnp.sum(earlier * onehot, axis=-1)


def local(
    queries,
    keys,
    values,
    cum_gate,
    doc_ids,
    residual,
    out_proj,
    norm_gain,
    route_ids,
    route_weights,
    expert_gate,
    expert_up,
    expert_down,
):
    own_tokens = queries.shape[0]
    head_count = queries.shape[1] // HEAD_DIM
    kv_count = keys.shape[1] // HEAD_DIM
    group_size = head_count // kv_count
    scale = HEAD_DIM ** (-0.5)
    own_start = lax.axis_index("sp") * own_tokens
    query_pos = own_start + jnp.arange(own_tokens, dtype=jnp.int32)
    query_heads = queries.reshape(own_tokens, kv_count, group_size, HEAD_DIM)
    query_gate = cum_gate.reshape(own_tokens, kv_count, group_size)
    gate_all, doc_all = (
        lax.all_gather(cum_gate, "sp", axis=0, tiled=True),
        lax.all_gather(doc_ids, "sp", axis=0, tiled=True),
    )

    def attend(state, key_block, value_block, first, block_len):
        gate_keys = lax.dynamic_slice_in_dim(gate_all, first, block_len, 0)
        doc_keys = lax.dynamic_slice_in_dim(doc_all, first, block_len, 0)
        key_heads = key_block.reshape(block_len, kv_count, HEAD_DIM)
        value_heads = value_block.reshape(block_len, kv_count, HEAD_DIM)
        scores = (
            jnp.einsum("tkgd,skd->tkgs", query_heads, key_heads, preferred_element_type=jnp.float32)
            * scale
        )
        scores = (
            scores
            + query_gate[..., None]
            - gate_keys.T.reshape(kv_count, group_size, block_len)[None]
        )
        key_pos = first + jnp.arange(block_len, dtype=jnp.int32)
        allowed = (key_pos[None, :] <= query_pos[:, None]) & (doc_keys[None, :] == doc_ids[:, None])
        allowed = allowed[:, None, None, :]
        scores = jnp.where(allowed, scores, very_low)
        top_old, total_old, summed_old = state
        top_new = jnp.maximum(top_old, jnp.max(scores, axis=-1))
        weights = jnp.where(allowed, jnp.exp(scores - top_new[..., None]), 0.0)
        fade = jnp.exp(top_old - top_new)
        total_new = total_old * fade + jnp.sum(weights, axis=-1)
        summed_new = summed_old * fade[..., None] + jnp.einsum(
            "tkgs,skd->tkgd",
            weights.astype(jnp.bfloat16),
            value_heads,
            preferred_element_type=jnp.float32,
        )
        return (top_new, total_new, summed_new)

    start_state = (
        jnp.full((own_tokens, kv_count, group_size), very_low, jnp.float32),
        jnp.zeros((own_tokens, kv_count, group_size), jnp.float32),
        jnp.zeros((own_tokens, kv_count, group_size, HEAD_DIM), jnp.float32),
    )
    key_piece = lax.all_gather(keys, "sp", axis=0, tiled=True)
    value_piece = lax.all_gather(values, "sp", axis=0, tiled=True)
    piece_len = key_piece.shape[0]
    block_len = min(piece_len, own_tokens)

    def one_block(index, inner):
        offset = index * block_len
        key_block = lax.dynamic_slice_in_dim(key_piece, offset, block_len, 0)
        value_block = lax.dynamic_slice_in_dim(value_piece, offset, block_len, 0)
        last_doc = lax.dynamic_index_in_dim(doc_all, offset + block_len - 1, 0, keepdims=False)
        needed = (offset <= own_start + own_tokens - 1) & (last_doc >= doc_ids[0])
        return lax.cond(
            needed,
            lambda carried: attend(carried, key_block, value_block, offset, block_len),
            lambda carried: carried,
            inner,
        )

    top, total, summed = lax.fori_loop(0, piece_len // block_len, one_block, start_state)
    attended = (
        (summed / total[..., None]).reshape(own_tokens, head_count * HEAD_DIM).astype(jnp.bfloat16)
    )
    sp_count = lax.axis_size("sp")
    rows_dev = residual.shape[0]
    plane_entries = lax.all_to_all(attended, "tp", split_axis=0, concat_axis=1, tiled=True)
    projected = jnp.dot(plane_entries, out_proj, preferred_element_type=jnp.float32)
    stream = (residual.astype(jnp.float32) + projected).astype(jnp.bfloat16)
    stream_f = stream.astype(jnp.float32)
    normed = stream_f * lax.rsqrt(jnp.mean(stream_f * stream_f, axis=1, keepdims=True) + norm_eps)
    normed = (normed * norm_gain[None, :]).astype(jnp.bfloat16)
    exp_dev = expert_gate.shape[0]
    experts = exp_dev * sp_count
    capacity = max(2, 2 * rows_dev * TOP // experts)
    own_flat = route_ids.reshape(-1)
    own_rank = slot_ranks(route_ids.reshape(1, rows_dev * TOP), experts)[0]
    own_dest = own_flat * capacity + own_rank
    row_of = jnp.arange(rows_dev * TOP, dtype=jnp.int32) // TOP
    outgoing = jnp.zeros((experts * capacity, D), jnp.bfloat16).at[own_dest].set(normed[row_of])
    arrived = lax.all_to_all(
        outgoing.reshape(experts, capacity, D), "sp", split_axis=0, concat_axis=1, tiled=True
    )
    arrived = arrived.reshape(exp_dev, sp_count, 1, capacity, D)
    piece = lax.all_gather(arrived, "tp", axis=2, tiled=True)
    gate = jnp.einsum("esncd,edf->esncf", piece, expert_gate, preferred_element_type=jnp.float32)
    upper = jnp.einsum("esncd,edf->esncf", piece, expert_up, preferred_element_type=jnp.float32)
    hidden = (jax.nn.silu(gate) * upper).astype(jnp.bfloat16)
    partial_value = jnp.einsum(
        "esncf,efd->esncd", hidden, expert_down, preferred_element_type=jnp.float32
    )
    expert_sums = lax.psum_scatter(
        partial_value.astype(jnp.bfloat16), "tp", scatter_dimension=2, tiled=True
    )
    expert_out = expert_sums.reshape(exp_dev, sp_count * capacity, D)
    returned = lax.all_to_all(expert_out, "sp", split_axis=1, concat_axis=0, tiled=True)
    selected = returned.reshape(experts * capacity, D)[own_dest]
    weighted = selected.astype(jnp.float32).reshape(rows_dev, TOP, D) * route_weights[..., None]
    return (stream_f + jnp.sum(weighted, axis=1)).astype(jnp.bfloat16)


def fused_kernel(
    q, kt, vt, gt, doc, res, gain, idt, wtt, wo_hbm, wg_hbm, wu_hbm, wd_hbm,
    base, mixed,
    wo, wg, wu, wd, qs, kvall, auxall, sc, mx, tot, acc, att, gath, proj, outg,
    xin, pc, r1, r3, ysum, ry, zsum, ret,
    wsem, kv_s, kv_r, ax_s, ax_r, kq_s, aq_s, at_s, at_r, d_s, d_r, fy_s, fy_r, fp_s, fp_r, fq_s, fq_r,
    c1_s, c1_r, c3_s, c3_r, cy_s, cy_r, cz_s, cz_r,
    *, n_sp, n_tp, cap,
):
    me = lax.axis_index("sp")
    t = lax.axis_index("tp")
    tok, width = q.shape
    heads = width // HEAD_DIM
    rows = res.shape[0]
    depth = res.shape[1]
    slots = n_sp * cap
    part = n_sp // 4
    flip = lambda k: t + k - 2 * k * (lax.div(t, k) % 2)
    partner = flip(1)
    across = flip(2)
    corner = 3 - t
    sib = me + 1 - 2 * lax.rem(me, 2)
    f32, bf16 = jnp.float32, jnp.bfloat16

    def remote(src, dst, ss, rs, dev):
        return pltpu.make_async_remote_copy(
            src_ref=src, dst_ref=dst, send_sem=ss, recv_sem=rs,
            device_id=dev, device_id_type=pl.DeviceIdType.MESH,
        )

    def peer_at(k):
        return lax.rem(me + k, n_sp)

    def swap_at(k):
        bits, at = [], 1
        while at < n_sp:
            bits.append((lax.rem(lax.div(k, at), 2), lax.rem(lax.div(me, at), 2), at))
            at *= 2
        want = [b[0] for b in bits]
        want[1], want[2] = want[2], want[1] + want[2] - 2 * want[1] * want[2]
        j = me
        for w, (_, m, p) in zip(want, bits):
            j = j + (w - 2 * w * m) * p
        return j

    def span(lo, hi, fn):
        def body(k, _):
            fn(k)
            return 0

        lax.fori_loop(lo, hi, body, 0)

    loads = [
        pltpu.make_async_copy(a, b, wsem.at[i])
        for i, (a, b) in enumerate(((wo_hbm, wo), (wg_hbm, wg), (wu_hbm, wu), (wd_hbm, wd)))
    ]
    for c in loads:
        c.start()
    kvall[me, :HEAD_DIM, :] = kt[...]
    kvall[me, HEAD_DIM:, :] = vt[...]
    auxall[me, :heads, :] = gt[...]
    auxall[me, heads : heads + 1, :] = doc[...].astype(f32)

    barrier = pltpu.get_barrier_semaphore()
    span(1, n_sp, lambda k: pl.semaphore_signal(
        barrier, inc=1, device_id=(peer_at(k), t), device_id_type=pl.DeviceIdType.MESH))
    for other in (partner, across, corner):
        pl.semaphore_signal(barrier, inc=1, device_id=(me, other), device_id_type=pl.DeviceIdType.MESH)

    def column(row, size):
        eye = lax.broadcasted_iota(jnp.int32, (size, size), 0) == lax.broadcasted_iota(
            jnp.int32, (size, size), 1
        )
        return jnp.sum(jnp.where(eye, jnp.broadcast_to(row, (size, size)), 0.0), axis=1, keepdims=True)

    qpos = lax.broadcasted_iota(jnp.int32, (tok, tok), 0)
    kpos = lax.broadcasted_iota(jnp.int32, (tok, tok), 1)
    qdoc = column(doc[...].astype(f32), tok)
    qgate = [column(gt[h : h + 1, :], tok) for h in range(heads)]
    scale = HEAD_DIM ** (-0.5)
    for h in range(heads):
        qs[h] = q[:, h * HEAD_DIM : (h + 1) * HEAD_DIM]
        mx[h] = jnp.full((tok, tok), very_low, f32)
        tot[h] = jnp.zeros((tok, tok), f32)
        acc[h] = jnp.zeros((tok, HEAD_DIM), f32)
    pl.semaphore_wait(barrier, n_sp - 1 + n_tp - 1)
    def kv_copies(to, frm):
        return (
            remote(kvall.at[frm], kvall.at[frm], kv_s.at[to], kv_r.at[frm], (to, t)),
            remote(auxall.at[frm], auxall.at[frm], ax_s.at[to], ax_r.at[frm], (to, t)),
        )

    def kv_relays(frm):
        return (
            remote(kvall.at[frm], kvall.at[frm], kq_s.at[frm], kv_r.at[frm], (sib, t)),
            remote(auxall.at[frm], auxall.at[frm], aq_s.at[frm], ax_r.at[frm], (sib, t)),
        )

    ahead = lax.div(n_sp - 1 - me, 2)

    def kv_out(do):
        def one(m):
            for c in kv_copies(me + 2 * (ahead - m), me):
                do(c)

        span(0, ahead, one)

        @pl.when(sib > me)
        def _():
            for c in kv_copies(sib, me):
                do(c)

    kv_out(lambda c: c.start())

    def score_block(j):
        kb = kvall[j, :HEAD_DIM, :]
        ax = auxall[j]
        allowed = (kpos + j * tok <= qpos + me * tok) & (ax[heads : heads + 1, :] == qdoc)
        for h in range(heads):
            s = jnp.dot(qs[h], kb, preferred_element_type=f32)
            s = s * scale + qgate[h] - ax[h : h + 1, :]
            s = jnp.where(allowed, s, very_low)
            sc[j, h] = s
            mx[h] = jnp.maximum(mx[h], s)

    score_block(me)

    def same_parity(m):
        j = me - 2 * m
        for c in kv_copies(j, j):
            c.wait_recv()
        for c in kv_relays(j):
            c.start()
        score_block(j)

    span(1, lax.div(me, 2) + 1, same_parity)

    def other_parity(m):
        j = me - 1 - 2 * m
        for c in kv_copies(j, j):
            c.wait_recv()
        score_block(j)

    span(0, lax.div(me + 1, 2), other_parity)
    for h in range(heads):
        mx[h] = jnp.broadcast_to(jnp.max(mx[h], axis=1, keepdims=True), (tok, tok))

    def second_pass(j):
        vb = kvall[j, HEAD_DIM:, :]
        for h in range(heads):
            e = jnp.exp(sc[j, h] - mx[h])
            tot[h] = tot[h] + e
            acc[h] = acc[h] + lax.dot_general(
                e.astype(bf16), vb, (((1,), (1,)), ((), ())), preferred_element_type=f32
            )

    span(0, me + 1, second_pass)
    pieces = [
        (acc[h] / jnp.sum(tot[h], axis=1, keepdims=True)).astype(bf16) for h in range(heads)
    ]
    att[...] = jnp.concatenate(pieces, axis=1)
    def att_copy(to, frm):
        return remote(
            att.at[pl.ds(pl.multiple_of(to * rows, rows), rows), :], gath.at[frm],
            at_s.at[to], at_r.at[frm], (me, to),
        )

    for other in (across, corner, partner):
        att_copy(other, t).start()
    gath[t] = att[pl.ds(pl.multiple_of(t * rows, rows), rows), :]

    srow = lax.broadcasted_iota(jnp.int32, (slots, rows), 0)
    named = ((idt[0:1, :] == srow // cap) | (idt[1:2, :] == srow // cap)).astype(f32)
    r_a = lax.broadcasted_iota(jnp.int32, (rows, rows), 0)
    r_b = lax.broadcasted_iota(jnp.int32, (rows, rows), 1)
    before = (r_a < r_b).astype(bf16)
    rank = jnp.dot(named.astype(bf16), before, preferred_element_type=f32)
    pick = jnp.where(rank == (srow % cap).astype(f32), named, 0.0).astype(bf16)
    lane = lax.broadcasted_iota(jnp.int32, (rows, slots), 1)
    owner = (lane // cap).astype(f32)
    back = [(column(idt[k : k + 1, :].astype(f32), rows) == owner).astype(f32) for k in range(TOP)]
    share = [column(wtt[k : k + 1, :], rows) for k in range(TOP)]
    after = (r_b < r_a).astype(bf16)
    rank_t = jnp.dot(after, (back[0] + back[1]).astype(bf16), preferred_element_type=f32)
    back = [jnp.where(rank_t == (lane % cap).astype(f32), b, 0.0).astype(bf16) for b in back]
    loads[0].wait()
    for i, src in enumerate((t, partner, across, corner)):
        if i:
            att_copy(src, src).wait_recv()
        term = jnp.dot(
            gath[src], wo[pl.ds(pl.multiple_of(src * width, width), width), :],
            preferred_element_type=f32,
        )
        proj[...] = term if i == 0 else proj[...] + term
    stream = (res[...].astype(f32) + proj[...]).astype(bf16)
    base[...] = stream
    stream_f = stream.astype(f32)
    normed = stream_f * lax.rsqrt(jnp.mean(stream_f * stream_f, axis=1, keepdims=True) + norm_eps)
    normed = (normed * gain[...]).astype(bf16)
    outg[...] = (
        jnp.dot(pick, normed, preferred_element_type=f32).astype(bf16).reshape(n_sp, cap, depth)
    )
    def out_copy(k):
        to = swap_at(k)
        return remote(outg.at[to], xin.at[t, k], d_s.at[k], d_r.at[k], (to, t))

    def to_across(k, line):
        return remote(xin.at[line, k], xin.at[line, k], fy_s.at[k], fy_r.at[k], (me, across))

    def to_partner(k, line):
        return remote(xin.at[line, k], xin.at[line, k], fp_s.at[k], fp_r.at[k], (me, partner))

    def relay_partner(k, line):
        return remote(xin.at[line, k], xin.at[line, k], fq_s.at[k], fq_r.at[k], (me, partner))

    def c1_copy(k):
        return remote(pc.at[partner, k], r1.at[k], c1_s.at[k], c1_r.at[k], (me, partner))

    def c3_copy(k):
        return remote(pc.at[corner, k], r3.at[k], c3_s.at[k], c3_r.at[k], (me, partner))

    def cy_copy(k):
        return remote(ysum.at[k], ry.at[k], cy_s.at[k], cy_r.at[k], (me, across))

    def cz_copy(k, frm):
        return remote(zsum.at[k], ret.at[frm], cz_s.at[k], cz_r.at[k], (swap_at(k), t))

    span(1, n_sp, lambda k: out_copy(k).start())
    xin[t, 0] = outg[me]
    to_across(0, t).start()
    to_partner(0, t).start()

    def relay(k):
        to_across(k, across).wait_recv()
        relay_partner(k, across).start()

    def forward(k):
        out_copy(k).wait_recv()
        to_across(k, t).start()
        to_partner(k, t).start()
        relay(k - 1)

    def expert(lo):
        x = xin[:, lo : lo + part].reshape(n_tp * part * cap, depth)
        g = jnp.dot(x, wg[...], preferred_element_type=f32)
        u = jnp.dot(x, wu[...], preferred_element_type=f32)
        hid = (g / (1.0 + jnp.exp(-g)) * u).astype(bf16)
        pc[:, lo : lo + part] = (
            jnp.dot(hid, wd[...], preferred_element_type=f32).astype(bf16).reshape(n_tp, part, cap, depth)
        )

    def pair_sum(k):
        c3_copy(k).wait_recv()
        ysum[k] = (pc[across, k].astype(f32) + r3[k].astype(f32)).astype(bf16)
        cy_copy(k).start()

    def full_sum(k):
        c1_copy(k).wait_recv()
        cy_copy(k).wait_recv()
        zsum[k] = (pc[t, k].astype(f32) + r1[k].astype(f32) + ry[k].astype(f32)).astype(bf16)

        @pl.when(k > 0)
        def _():
            cz_copy(k, me).start()

    def arrive(k):
        to_partner(k, partner).wait_recv()
        relay_partner(k, corner).wait_recv()

    def hand_over(k):
        c3_copy(k).start()
        c1_copy(k).start()

    for step in range(7):
        lo = step * part
        if step < 4:
            span(max(lo, 1), lo + part, forward)
        if step == 4:
            relay(n_sp - 1)
        lo = (step - 2) * part
        if 0 <= lo < n_sp:
            span(lo, lo + part, pair_sum)
        lo = (step - 3) * part
        if 0 <= lo < n_sp:
            span(lo, lo + part, full_sum)
        lo = (step - 1) * part
        if 0 <= lo < n_sp:
            if step == 1:
                for c in loads[1:]:
                    c.wait()
            span(lo, lo + part, arrive)
            expert(lo)
            span(lo, lo + part, hand_over)
    ret[me] = zsum[0]
    span(1, n_sp, lambda k: cz_copy(k, swap_at(k)).wait_recv())
    got = ret[...].reshape(slots, depth)
    mix = share[0] * jnp.dot(back[0], got, preferred_element_type=f32)
    for k in range(1, TOP):
        mix = mix + share[k] * jnp.dot(back[k], got, preferred_element_type=f32)
    mixed[...] = mix
    kv_out(lambda c: c.wait_send())

    def end_relay(m):
        for c in kv_relays(me - 2 * m):
            c.wait_send()

    span(1, lax.div(me, 2) + 1, end_relay)
    for other in (across, corner, partner):
        att_copy(other, t).wait_send()

    def end_peers(k):
        out_copy(k).wait_send()
        cz_copy(k, me).wait_send()

    span(1, n_sp, end_peers)

    def end_all(k):
        to_across(k, t).wait_send()
        to_partner(k, t).wait_send()
        relay_partner(k, across).wait_send()
        c1_copy(k).wait_send()
        c3_copy(k).wait_send()
        cy_copy(k).wait_send()

    span(0, n_sp, end_all)


def fused(
    queries, keys, values, cum_gate, doc_ids, residual, out_proj, norm_gain,
    route_ids, route_weights, expert_gate, expert_up, expert_down,
):
    n_sp, n_tp = lax.axis_size("sp"), lax.axis_size("tp")
    tok, width = queries.shape
    heads = width // HEAD_DIM
    rows, depth = residual.shape
    cap = max(2, 2 * rows * TOP // n_sp)
    ff = expert_gate.shape[2]
    slots = n_sp * cap
    f32, bf16 = jnp.float32, jnp.bfloat16
    height = -(-(heads + 1) // 8) * 8
    vm = pl.BlockSpec(memory_space=pltpu.VMEM)
    hb = pl.BlockSpec(memory_space=pl.ANY)
    block = pltpu.VMEM((n_sp, cap, depth), bf16)
    dma = lambda n: pltpu.SemaphoreType.DMA((n,))
    call = pl.pallas_call(
        functools.partial(fused_kernel, n_sp=n_sp, n_tp=n_tp, cap=cap),
        out_shape=(
            jax.ShapeDtypeStruct((rows, depth), bf16),
            jax.ShapeDtypeStruct((rows, depth), f32),
        ),
        in_specs=[vm] * 9 + [hb] * 4,
        out_specs=(vm, vm),
        scratch_shapes=[
            pltpu.VMEM(out_proj.shape, bf16),
            pltpu.VMEM((depth, ff), bf16),
            pltpu.VMEM((depth, ff), bf16),
            pltpu.VMEM((ff, depth), bf16),
            pltpu.VMEM((heads, tok, HEAD_DIM), bf16),
            pltpu.VMEM((n_sp, 2 * HEAD_DIM, tok), bf16),
            pltpu.VMEM((n_sp, height, tok), f32),
            pltpu.VMEM((n_sp, heads, tok, tok), f32),
            pltpu.VMEM((heads, tok, tok), f32),
            pltpu.VMEM((heads, tok, tok), f32),
            pltpu.VMEM((heads, tok, HEAD_DIM), f32),
            pltpu.VMEM((tok, width), bf16),
            pltpu.VMEM((n_tp, rows, width), bf16),
            pltpu.VMEM((rows, depth), f32),
            block,
            pltpu.VMEM((n_tp, n_sp, cap, depth), bf16),
        ]
        + [pltpu.VMEM((n_tp, n_sp, cap, depth), bf16)]
        + [block] * 6
        + [dma(4)]
        + [dma(n_sp)] * 6
        + [dma(n_tp)] * 2
        + [dma(n_sp)] * 16,
        compiler_params=pltpu.CompilerParams(
            collective_id=0, has_side_effects=True, vmem_limit_bytes=60 * 1024 * 1024
        ),
    )
    base, mixed = call(
        queries, keys.T, values.T, cum_gate.T, doc_ids.reshape(1, tok), residual, norm_gain.reshape(1, depth),
        route_ids.T, route_weights.T, out_proj, expert_gate[0], expert_up[0], expert_down[0],
    )
    return (base.astype(f32) + mixed).astype(bf16)


def chosen(*args):
    n_sp, n_tp = lax.axis_size("sp"), lax.axis_size("tp")
    queries, keys, residual, expert_gate = args[0], args[1], args[5], args[10]
    cap = max(2, 2 * residual.shape[0] * TOP // n_sp)
    fits = (
        n_tp == 4
        and n_sp >= 8
        and n_sp & (n_sp - 1) == 0
        and expert_gate.shape[0] == 1
        and keys.shape[1] == HEAD_DIM
        and queries.shape[0] == 128
        and cap % 16 == 0
        and residual.shape[0] % 32 == 0
    )
    return fused(*args) if fits else local(*args)


def solution(mesh):
    in_specs = (
        P("sp", "tp"),
        P("sp", "tp"),
        P("sp", "tp"),
        P("sp", "tp"),
        P("sp"),
        P(("sp", "tp"), None),
        P(),
        P(),
        P(("sp", "tp"), None),
        P(("sp", "tp"), None),
        P("sp", None, "tp"),
        P("sp", None, "tp"),
        P("sp", "tp", None),
    )
    out_specs = P(("sp", "tp"), None)
    return jax.shard_map(chosen, mesh=mesh, in_specs=in_specs, out_specs=out_specs, check_vma=False)
```
